32 devices in a mesh: sp: 8 (over z, y), dp: 4 (over x, core).
Axes of the slice: x: 2, y: 2, z: 4, core: 2. Of those that a mesh axis runs over, the one named last changes fastest.
Arguments:
- queries: bfloat16 [4, 1024, 1024], P('dp', 'sp'), may hold values from -6 to 6
- keys: bfloat16 [4, 1024, 256], P('dp', 'sp'), may hold values from -6 to 6
- values: bfloat16 [4, 1024, 256], P('dp', 'sp'), may hold values from -6 to 6
- q_gain: float32 [64], replicated, may hold values from 0.55 to 8
- k_gain: float32 [64], replicated, may hold values from 0.55 to 8
- residual: bfloat16 [4, 1024, 2048], P('dp', 'sp'), may hold values from -6 to 6
- out_weight: bfloat16 [1024, 2048], replicated, may hold values from -0.1875 to 0.1875
- mix_gain: float32 [2048], replicated, may hold values from 0.1 to 1.9
- ffn_gain: float32 [2048], replicated, may hold values from 0.1 to 1.9
- post_gain: float32 [2048], replicated, may hold values from 0.1 to 1.9
- expert_ids: int32 [4, 1024, 2], P('dp', 'sp'), may hold values from 0 to 31, all different within a row; in each aligned block of 128 rows (0 to 127, 128 to 255, ..., all dimensions but the last counted through in order) at most 16 rows name the same one
- expert_gate: float32 [4, 1024, 2], P('dp', 'sp'), may hold values from 0.05 to 1
- w_gate: bfloat16 [32, 2048, 512], P(('sp', 'dp')), may hold values from -0.125 to 0.125
- w_up: bfloat16 [32, 2048, 512], P(('sp', 'dp')), may hold values from -0.125 to 0.125
- w_down: bfloat16 [32, 512, 2048], P(('sp', 'dp')), may hold values from -0.25 to 0.25
Outputs:
- result: bfloat16 [4, 1024, 2048], P('dp', 'sp')
The draws below stay inside these ranges and needn't reach their ends.
Inputs may be any that keep to these rules, and one draw needn't show every extreme that they name: `expert_ids`: each token names 2 different experts; among the 128 tokens of one device no expert is named more than 16 times, and that bound is reached.
All inputs are finite; a program needn't handle non-finite values.
Results may differ from the reference program's by a relative error of at most 0.0085.
The reference program's roundings to bfloat16 on the way count: a program that leaves them out, or rounds other values in their place, can miss the bound.
Values may be sent and summed in bfloat16 or wider, within the bound.
A program may use at most 64 MiB of HBM per device.

```python
import math
import jax
import jax.numpy as jnp
import numpy as np
from jax import lax

D = 2048
HEAD = 64
H_Q = 16
H_KV = 4
DE = 512
TOP = 2
GRID = 64
TOK_DEV = 128
SEQS = 4
LEN = 1024
EXPERTS = 32
CAP = 16
N_SP = 8
N_DP = 4


def key_field(key):
    base = jax.random.normal(jax.random.fold_in(key, 23), (SEQS, LEN, H_KV * HEAD), jnp.float32)
    return jnp.clip(base, -6.0, 6.0)


def draw_keys(key, part):
    return key_field(key).astype(jnp.bfloat16)


def draw_queries(key, part):
    base = jax.random.normal(jax.random.fold_in(key, 11), (SEQS, LEN, H_Q * HEAD), jnp.float32)
    base = jnp.clip(base, -6.0, 6.0)
    return base.astype(jnp.bfloat16)


def draw_q_gain(key, part):
    inner = jax.random.fold_in(key, 41)
    return 1.0 + 0.18 * jnp.clip(jax.random.normal(inner, (HEAD,), jnp.float32), -2.5, 2.5)


def draw_k_gain(key, part):
    inner = jax.random.fold_in(key, 43)
    return 1.0 + 0.18 * jnp.clip(jax.random.normal(inner, (HEAD,), jnp.float32), -2.5, 2.5)


def level_of(own_key, dims, pieces, least, largest):
    level = 1.0
    for dim, blocks in pieces:
        draws = jax.random.uniform(jax.random.fold_in(jax.random.fold_in(own_key, 6), dim), (blocks,), jnp.float32, least / len(pieces), largest / len(pieces))
        level = level * jnp.repeat(jnp.exp(draws), dims[dim] // blocks).reshape((-1,) + (1,) * (len(dims) - 1 - dim))
    return level


def routed_block(own_key, own, number, rows, count, top, reach, lean):
    ranking = jax.random.permutation(own_key, count)
    crowded, ordinary = load_shares(count, rows * top, reach, lean, True), load_shares(count, rows * top, reach, lean, False)
    places = jnp.arange(count)

    def named(lengths, turn):
        used = int((lengths > 0).sum())
        fixed = max(1, used // 4)
        passed = fixed + (places - fixed + turn * (used - fixed)) % max(1, count - fixed)
        return jnp.zeros((count,), jnp.int32).at[ranking[jnp.where(places < fixed, places, passed)]].set(jnp.asarray(lengths, jnp.int32))

    lengths = jnp.where(number % 4 == 0, named(crowded, number // 4), named(ordinary, number - number // 4 - 1))
    mixed = jax.random.permutation(jax.random.fold_in(own, 3), count)
    giver, sink = mixed[0:count // 2 * 2:2], mixed[1:count // 2 * 2:2]
    slack = jnp.minimum(lengths[giver] - 1, reach - lengths[sink]) // 2
    slack = jnp.where((giver == ranking[0]) | (sink == ranking[0]) | (lengths[sink] == 0), 0, jnp.maximum(slack, 0))
    passed = jax.random.randint(jax.random.fold_in(own, 4), (count // 2,), 0, 1 << 20) % (slack + 1)
    lengths = lengths.at[giver].add(-passed).at[sink].add(passed)
    members = jnp.searchsorted(jnp.cumsum(lengths), jnp.arange(rows * top), side="right").astype(jnp.int32)
    listing = members.reshape(top, rows).T
    listing = listing[jax.random.permutation(jax.random.fold_in(own, 1), rows)]
    turn = jax.random.randint(jax.random.fold_in(own, 2), (rows, 1), 0, top)
    return jnp.take_along_axis(listing, (jnp.arange(top)[None, :] + turn) % top, axis=1)


def load_shares(number_of, total, most, slope, full):
    portions = [(1 << 20) // math.isqrt(grade ** slope) + 1 for grade in range(1, number_of + 1)]
    largest = most if full else min(most, max(-(-total // number_of), total * portions[0] // sum(portions)))
    least = 1 if total - largest >= number_of - 1 else 0
    holding, spare = [largest] + [least] * (number_of - 1), total - largest - least * (number_of - 1)
    while spare > 0:
        movable = [i for i in range(1, number_of) if holding[i] < largest] or [i for i in range(1, number_of) if holding[i] < most]
        mass, left = sum([portions[i] for i in movable]), spare
        for i in movable:
            addition = min(most - holding[i], max(1, left * portions[i] // mass), spare)
            holding[i] = holding[i] + addition
            spare = spare - addition
    return np.array(holding)


def scatter_about(stream_key, dims, width, bound, cuts=(), kind=jnp.bfloat16):
    drawn = width * jax.random.normal(stream_key, dims, jnp.float32)
    if cuts:
        drawn = drawn * level_of(stream_key, dims, cuts, -0.22, 0.18)
    return jnp.clip(drawn, -bound, bound).astype(kind)


def setup_inputs(seed: int = 0) -> dict:
    splits = jax.random.split(jax.random.key(seed), 16)
    queries = draw_queries(jax.random.fold_in(splits[15], 71), 0)
    keys = draw_keys(jax.random.fold_in(splits[15], 71), 0)
    values = scatter_about(splits[2], (SEQS, LEN, H_KV * HEAD), 1.0, 6.0, ((0, 4), (1, 8)))
    q_gain = draw_q_gain(jax.random.fold_in(splits[15], 71), 0)
    k_gain = draw_k_gain(jax.random.fold_in(splits[15], 71), 0)
    residual = scatter_about(splits[5], (SEQS, LEN, D), 1.0, 6.0, ((0, 4), (1, 8)))
    out_weight = scatter_about(splits[6], (H_Q * HEAD, D), (H_Q * HEAD) ** -0.5, 0.1875)
    mix_gain = jnp.clip(1.0 + 0.18 * jax.random.normal(splits[7], (D,), jnp.float32), 0.1, 1.9)
    ffn_gain = jnp.clip(1.0 + 0.18 * jax.random.normal(splits[8], (D,), jnp.float32), 0.1, 1.9)
    post_gain = jnp.clip(1.0 + 0.18 * jax.random.normal(splits[9], (D,), jnp.float32), 0.1, 1.9)
    expert_ids_keys = jax.random.split(jax.random.fold_in(splits[10], 1), SEQS * LEN // TOK_DEV)
    expert_ids_turns = jax.random.permutation(jax.random.fold_in(splits[10], 3), SEQS * LEN // TOK_DEV)
    expert_ids = jax.vmap(lambda own, number: routed_block(jax.random.fold_in(splits[10], 2), own, number, TOK_DEV, EXPERTS, TOP, CAP, 2))(expert_ids_keys, expert_ids_turns).reshape((SEQS, LEN, TOP))
    expert_gate = jnp.clip(jnp.exp(math.log(1.0) - 2.9957323 * jax.random.uniform(splits[11], (SEQS, LEN, TOP), jnp.float32) ** level_of(splits[11], (SEQS, LEN, TOP), ((0, 4), (1, 8)), -0.2, 0.2)), 0.05, 1.0)
    w_gate = scatter_about(splits[12], (EXPERTS, D, DE), D ** -0.5, 0.125, ((0, 32),))
    w_up = scatter_about(splits[13], (EXPERTS, D, DE), D ** -0.5, 0.125, ((0, 32),))
    w_down = scatter_about(splits[14], (EXPERTS, DE, D), DE ** -0.5, 0.25, ((0, 32),))
    return {"queries": queries, "keys": keys, "values": values, "q_gain": q_gain, "k_gain": k_gain, "residual": residual, "out_weight": out_weight, "mix_gain": mix_gain, "ffn_gain": ffn_gain, "post_gain": post_gain, "expert_ids": expert_ids, "expert_gate": expert_gate, "w_gate": w_gate, "w_up": w_up, "w_down": w_down}


eps_norm = 1e-06
theta_base = 10000.0
block_rows = 512

def rms_scale(values):
    return values * lax.rsqrt(lax.optimization_barrier(jnp.mean(values * values, axis=-1, keepdims=True)) + eps_norm)

def rotate(field, gain):
    seq_len, head_count, head_size = field.shape
    values = rms_scale(field.astype(jnp.float32)) * gain
    positions = jnp.arange(seq_len, dtype=jnp.int32)
    row_index = (positions // GRID).astype(jnp.float32)
    col_index = (positions % GRID).astype(jnp.float32)
    pair_quarter = head_size // 4
    frequency = theta_base ** (-(4.0 * jnp.arange(pair_quarter, dtype=jnp.float32)) / head_size)
    angles = jnp.concatenate([row_index[:, None] * frequency, col_index[:, None] * frequency], axis=1)
    cosine_table = jnp.cos(angles)[:, None, :]
    sine_table = jnp.sin(angles)[:, None, :]
    paired = values.reshape(seq_len, head_count, head_size // 2, 2)
    even_part = paired[..., 0]
    odd_part = paired[..., 1]
    turned = jnp.stack([even_part * cosine_table - odd_part * sine_table, even_part * sine_table + odd_part * cosine_table], axis=-1)
    return turned.reshape(seq_len, head_count, head_size).astype(jnp.bfloat16)

def attend(q_turned, k_turned, v_rows):
    seq_len, q_count, head_size = q_turned.shape
    kv_count = k_turned.shape[1]
    group_size = q_count // kv_count
    k_float = k_turned.astype(jnp.float32)
    v_float = v_rows.astype(jnp.float32)

    def one_block(start):
        q_block = lax.dynamic_slice_in_dim(q_turned, start, block_rows, 0)
        q_block = q_block.reshape(block_rows, kv_count, group_size, head_size).astype(jnp.float32)
        scores = jnp.einsum('qkgd,skd->kgqs', q_block, k_float) * head_size ** (-0.5)
        row_max = lax.optimization_barrier(jnp.max(scores, axis=-1, keepdims=True))
        exp_scores = jnp.exp(scores - row_max)
        weights = (exp_scores / lax.optimization_barrier(jnp.sum(exp_scores, axis=-1, keepdims=True))).astype(jnp.bfloat16)
        summed = jnp.einsum('kgqs,skd->qkgd', weights.astype(jnp.float32), v_float)
        return summed.astype(jnp.bfloat16).reshape(block_rows, q_count * head_size)
    starts = jnp.arange(seq_len // block_rows, dtype=jnp.int32) * block_rows
    return lax.map(one_block, starts).reshape(seq_len, q_count * head_size)

def reference(queries, keys, values, q_gain, k_gain, residual, out_weight, mix_gain, ffn_gain, post_gain, expert_ids, expert_gate, w_gate, w_up, w_down):
    seq_count, seq_len, q_width = queries.shape
    head_size = q_gain.shape[0]

    def per_sequence(items):
        q_seq, k_seq, v_seq = items
        q_turned = rotate(q_seq.reshape(seq_len, -1, head_size), q_gain)
        k_turned = rotate(k_seq.reshape(seq_len, -1, head_size), k_gain)
        return attend(q_turned, k_turned, v_seq.reshape(seq_len, -1, head_size))
    attended = lax.map(per_sequence, (queries, keys, values)).reshape(-1, q_width)
    projected = jnp.dot(attended, out_weight, preferred_element_type=jnp.float32)
    first_res = (residual.reshape(-1, D).astype(jnp.float32) + rms_scale(projected) * mix_gain).astype(jnp.bfloat16)
    normed = (rms_scale(first_res.astype(jnp.float32)) * ffn_gain).astype(jnp.bfloat16)
    flat_ids = expert_ids.reshape(-1).astype(jnp.int32)
    flat_gate = expert_gate.reshape(-1)
    slot_count = N_SP * N_DP * CAP

    def per_expert(running_sum, number):
        matches = flat_ids == number
        picked = jnp.nonzero(matches, size=slot_count, fill_value=0)[0].astype(jnp.int32)
        live_mask = (jnp.arange(slot_count, dtype=jnp.int32) < jnp.sum(matches.astype(jnp.int32))).astype(jnp.float32)
        token_rows = (picked // TOP).astype(jnp.int32)
        inputs = normed[token_rows]
        gate_value = jnp.dot(inputs, w_gate[number], preferred_element_type=jnp.float32)
        up_value = jnp.dot(inputs, w_up[number], preferred_element_type=jnp.float32)
        hidden = (jax.nn.silu(gate_value) * up_value).astype(jnp.bfloat16)
        expert_out = jnp.dot(hidden, w_down[number], preferred_element_type=jnp.float32).astype(jnp.bfloat16)
        weight = flat_gate[picked] * live_mask
        return (running_sum.at[token_rows].add(weight[:, None] * expert_out.astype(jnp.float32)), None)
    expert_sum, _ = lax.scan(per_expert, jnp.zeros((normed.shape[0], D), jnp.float32), jnp.arange(EXPERTS, dtype=jnp.int32))
    result = (first_res.astype(jnp.float32) + rms_scale(expert_sum) * post_gain).astype(jnp.bfloat16)
    return result.reshape(seq_count, seq_len, D)
```

```python
import functools

import jax
import jax.numpy as jnp
import numpy as np
from jax import lax
from jax.experimental import pallas as pl
from jax.experimental.pallas import tpu as pltpu
from jax.sharding import PartitionSpec as P

GRID = 64
LANES = 128
eps_norm = 1e-06
theta_base = 10000.0
MESH = pl.DeviceIdType.MESH
f32 = jnp.float32
bf16 = jnp.bfloat16


def tables(rows, head_size):
    half = head_size // 2
    lane = np.arange(LANES) % head_size
    pair = lane // 2
    quarter = head_size // 4
    by_row = pair < quarter
    frequency = theta_base ** (-(4.0 * (pair % quarter)) / head_size)
    sign = np.where(lane % 2 == 0, -1.0, 1.0)
    a_row = np.arange(rows)[:, None] * frequency
    a_col = np.arange(GRID)[:, None] * frequency
    out = (
        np.where(by_row, np.cos(a_row), 0.0),
        np.where(by_row, np.sin(a_row) * sign, 0.0),
        np.where(by_row, 0.0, np.cos(a_col)),
        np.where(by_row, 0.0, np.sin(a_col) * sign),
    )
    return [jnp.asarray(t, f32) for t in out]


def rms(x):
    return x * lax.rsqrt(jnp.mean(x * x, axis=-1, keepdims=True) + eps_norm)


def dot(a, b):
    return jnp.dot(a, b, preferred_element_type=f32)


def kernel(
    n_sp, n_dp, pitch, n_col,
    q_ref, k_ref, v_ref, qg_ref, kg_ref, cr_ref, sr_ref, cc_ref, sc_ref,
    res_ref, mix_ref, ffn_ref, post_ref, ids_ref, gate_ref,
    wo_hbm, wg_hbm, wu_hbm, wd_hbm,
    out_ref,
    kbuf, vbuf, att, first, rows, outbox, arrived, returned, pack, comb_hi, comb_lo,
    ids_far, gate_far, part, relayed, incoming, total,
    wo, wg, wu, wd, w_sem,
    kz_send, ky_send, k_recv, t_send, t_recv, z_send, z_recv,
    d_send, d_recv, r_send, r_recv, p_send, m_recv, i_recv,
):
    sp = lax.axis_index("sp")
    dp = lax.axis_index("dp")
    tok, q_width = q_ref.shape
    kv_width = k_ref.shape[1]
    head = qg_ref.shape[1]
    d_model = res_ref.shape[1]
    heads_q, heads_kv = q_width // head, kv_width // head
    group = heads_q // heads_kv

    weights = [
        pltpu.make_async_copy(src, dst, w_sem.at[n])
        for n, (src, dst) in enumerate(((wo_hbm, wo), (wg_hbm, wg), (wu_hbm, wu), (wd_hbm, wd)))
    ]
    for w in weights:
        w.start()

    wide = n_dp // 2
    planes = n_sp // wide
    n_pl = wide * n_dp
    n_slot = n_pl * pitch
    cols_c = d_model // n_col
    z = sp // wide
    y = sp % wide
    mid = (z // 2 + z % 2) % 2
    near = z + 1 - 2 * (z % 2)
    across = (z + 2) % planes
    mirror = planes - 1 - z
    is_mid = mid == 1
    is_end = mid == 0

    def at(plane):
        return plane * wide + y, dp

    def peer(i):
        return z * wide + lax.rem(y + i // n_dp, wide), lax.rem(dp + i % n_dp, n_dp)

    def source(i):
        return z * wide + lax.rem(y + wide - i // n_dp, wide), lax.rem(dp + n_dp - i % n_dp, n_dp)

    def remote(src, dst, s_sem, r_sem, to):
        return pltpu.make_async_remote_copy(src, dst, s_sem, r_sem, device_id=to, device_id_type=MESH)

    barrier = pltpu.get_barrier_semaphore()
    up_ok, down_ok = z < planes - 1, z > 0

    @pl.when(up_ok)
    def _():
        pl.semaphore_signal(barrier, inc=1, device_id=at(z + 1), device_id_type=MESH)

    @pl.when(down_ok)
    def _():
        pl.semaphore_signal(barrier, inc=1, device_id=at(z - 1), device_id_type=MESH)

    def greet(i, c):
        pl.semaphore_signal(barrier, inc=1, device_id=peer(i), device_id_type=MESH)
        return c

    lax.fori_loop(1, n_pl, greet, 0)

    lane = lax.broadcasted_iota(jnp.int32, (tok, LANES), 1)
    even = lane % 2 == 0
    low = lane % (2 * head) < head
    same = (
        lax.broadcasted_iota(jnp.int32, (LANES, LANES), 0) // head
        == lax.broadcasted_iota(jnp.int32, (LANES, LANES), 1) // head
    ).astype(bf16)
    per_dev = tok // GRID
    cos_t = jnp.concatenate(
        [cc_ref[...] + cr_ref[pl.ds(sp * per_dev + u, 1), :] for u in range(per_dev)], axis=0
    )
    sin_t = jnp.concatenate(
        [sc_ref[...] + sr_ref[pl.ds(sp * per_dev + u, 1), :] for u in range(per_dev)], axis=0
    )

    def turn(x, gain):
        x = x.astype(f32)
        square = x * x
        hi = square.astype(bf16)
        lo = (square - hi.astype(f32)).astype(bf16)
        mean = (dot(hi, same) + dot(lo, same)) * (1.0 / head)
        x = x * lax.rsqrt(mean + eps_norm) * gain
        swapped = jnp.where(even, pltpu.roll(x, LANES - 1, 1), pltpu.roll(x, 1, 1))
        return x * cos_t + swapped * sin_t

    k_gain = jnp.concatenate([kg_ref[...]] * (LANES // head), axis=1)
    q_gain = jnp.concatenate([qg_ref[...]] * (LANES // head), axis=1)
    for c in range(kv_width // LANES):
        cols = slice(c * LANES, (c + 1) * LANES)
        kbuf[sp, :, cols] = turn(k_ref[:, cols], k_gain).astype(bf16)
    vbuf[sp] = v_ref[...]

    pl.semaphore_wait(barrier, n_pl - 1 + jnp.minimum(z, 1) + jnp.minimum(planes - 1 - z, 1))

    bufs = (kbuf, vbuf)

    def block(kv, plane, own):
        return v_ref if own and kv == 1 else bufs[kv].at[plane * wide + y]

    def along(kv, up, t):
        plane, to = (z - (t - 1), z + 1) if up else (z + (t - 1), z - 1)
        return remote(
            block(kv, plane, t == 1), bufs[kv].at[plane * wide + y],
            kz_send.at[kv, up, t], k_recv.at[kv, plane * wide + y], at(to),
        )

    def aside(kv, plane, j, own=False):
        return remote(
            block(kv, plane, own), bufs[kv].at[plane * wide + y],
            ky_send.at[kv, plane, j], k_recv.at[kv, plane * wide + y],
            (z * wide + lax.rem(y + j, wide), dp),
        )

    def landed(kv, where):
        ref = bufs[kv].at[where]
        remote(ref, ref, kz_send.at[kv, 0, 0], k_recv.at[kv, where], at(z)).wait_recv()

    def along_ok(up, t):
        return (z >= t - 1) & up_ok if up else (z + t - 1 < planes) & down_ok

    def along_start(kv, up, t):
        @pl.when(along_ok(up, t))
        def _():
            along(kv, up, t).start()

    for kv in (1, 0):
        along_start(kv, 1, 1)
        along_start(kv, 0, 1)
        for j in range(1, wide):
            aside(kv, z, j, own=True).start()

    q_rows = [[] for _ in range(heads_kv)]
    per_chunk = LANES // head

    def turn_q(c):
        x = turn(q_ref[:, c * LANES : (c + 1) * LANES], q_gain) * head ** (-0.5)
        for part_ in range(per_chunk):
            kv = (c * per_chunk + part_) // group
            want = kv % per_chunk
            yq = x if part_ == want else pltpu.roll(x, head, 1)
            keep = low if want == 0 else jnp.logical_not(low)
            q_rows[kv].append(jnp.where(keep, yq, 0.0).astype(bf16))

    order = lax.broadcasted_iota(jnp.int32, (n_pl, tok), 0)
    e_iota = z * n_pl + (y + order // n_dp) % wide * n_dp + (dp + order % n_dp) % n_dp
    before = (
        lax.broadcasted_iota(jnp.int32, (tok, tok), 0) < lax.broadcasted_iota(jnp.int32, (tok, tok), 1)
    ).astype(bf16)
    spread = (
        lax.broadcasted_iota(jnp.int32, (n_slot, n_pl), 0) // pitch
        == lax.broadcasted_iota(jnp.int32, (n_slot, n_pl), 1)
    ).astype(bf16)
    place = (lax.broadcasted_iota(jnp.int32, (n_slot, tok), 0) % pitch + 1).astype(f32)

    def route(n, ids, gates):
        hit0 = (e_iota == ids[0:1, :]).astype(f32)
        hit1 = (e_iota == ids[1:2, :]).astype(f32)
        hits = hit0 + hit1
        rank = dot(hits.astype(bf16), before)
        mark = (hits * (rank + 1.0)).astype(bf16)
        chosen = dot(spread, mark) == place
        pack[n] = chosen.astype(f32).astype(bf16)
        g_hi = gates.astype(bf16).astype(f32)
        g_lo = gates - g_hi
        for dst, piece_ in ((comb_hi, g_hi), (comb_lo, g_lo)):
            both = (hit0 * piece_[0:1, :] + hit1 * piece_[1:2, :]).astype(bf16)
            dst[n] = jnp.where(chosen, dot(spread, both), 0.0).astype(bf16)

    n_turn = q_width // LANES
    done = 0
    for t in range(1, planes):
        upto = n_turn * t // (planes - 1)
        for c in range(done, upto):
            turn_q(c)
        done = upto
        if t == planes - 1:
            route(0, ids_ref[...], gate_ref[...])
        for kv in (1, 0):
            for up in (1, 0):
                plane = z - t if up else z + t

                @pl.when((z >= t) if up else (z + t < planes))
                def _():
                    landed(kv, plane * wide + y)
                    if t < planes - 1:
                        along_start(kv, up, t + 1)
                    for j in range(1, wide):
                        aside(kv, plane, j).start()

    def tables_to(n, to):
        return [
            remote(ids_ref, ids_far.at[n], t_send.at[0, n], t_recv.at[0, n], at(to)),
            remote(gate_ref, gate_far.at[n], t_send.at[1, n], t_recv.at[1, n], at(to)),
        ]

    tables_far = [c for n, to in ((1, near), (2, across), (3, mirror)) for c in tables_to(n, to)]
    for copy in tables_far:
        copy.start()

    for kv in (1, 0):
        for plane in range(planes):
            for j in range(1, wide):
                landed(kv, plane * wide + lax.rem(y + wide - j, wide))

    keys = n_sp * tok
    outs = {}
    for kv in range(heads_kv):
        cols = slice(kv // per_chunk * LANES, (kv // per_chunk + 1) * LANES)
        k_all = kbuf[:, :, cols].reshape(keys, LANES)
        v_all = vbuf[:, :, cols].reshape(keys, LANES)
        for part_ in range(group):
            s = lax.dot_general(
                q_rows[kv][part_], k_all, (((1,), (1,)), ((), ())), preferred_element_type=f32
            )
            p = jnp.exp(s - jnp.max(s, axis=-1, keepdims=True))
            denom = jnp.sum(p, axis=-1, keepdims=True)
            outs[kv * group + part_] = dot(p.astype(bf16), v_all) / denom
    for c in range(q_width // LANES):
        piece = None
        for part_ in range(per_chunk):
            h = c * per_chunk + part_
            have = (h // group) % per_chunk
            yo = outs[h] if part_ == have else pltpu.roll(outs[h], head, 1)
            piece = yo if piece is None else jnp.where(low, piece, yo)
        att[:, c * LANES : (c + 1) * LANES] = piece.astype(bf16)

    weights[0].wait()
    projected = dot(att[...], wo[...])
    mixed = (res_ref[...].astype(f32) + rms(projected) * mix_ref[...]).astype(bf16)
    first[...] = mixed
    normed = (rms(mixed.astype(f32)) * ffn_ref[...]).astype(bf16)
    chunks = range(n_col)

    def span(c):
        return slice(c * cols_c, (c + 1) * cols_c)

    for c in chunks:
        rows[0, c] = normed[:, span(c)]

    slots = (0, 1, 2 + mid, 3 - mid)
    beyond = mid * mirror + (1 - mid) * across

    def to_near(c):
        return remote(rows.at[0, c], rows.at[1, c], z_send.at[0, c], z_recv.at[1, c], at(near))

    def to_beyond(c):
        return remote(
            rows.at[0, c], rows.at[slots[2], c], z_send.at[1, c], z_recv.at[slots[2], c], at(beyond)
        )

    def pass_on(s, c):
        return remote(
            rows.at[5 - s, c], rows.at[s, c], z_send.at[s, c], z_recv.at[s, c], at(near)
        )

    def rows_landed(slot, c):
        remote(
            rows.at[slot, c], rows.at[slot, c], z_send.at[0, c], z_recv.at[slot, c], at(near)
        ).wait_recv()

    def relay(s):
        @pl.when(is_mid)
        def _():
            for c in chunks:
                rows_landed(slots[s], c)
                pass_on(s, c).start()

    def dispatch(s, c, i):
        q = slots[s]
        return remote(
            outbox.at[q, c, i], arrived.at[q, c, i], d_send.at[q, c], d_recv.at[q, c], peer(i)
        )

    def answer(s, c, i):
        q = slots[s]
        return remote(
            arrived.at[q, c, i], returned.at[q, c, i], r_send.at[q, c], r_recv.at[q, c], source(i)
        )

    def start_all(make, s, c):
        def step(i, carry):
            make(s, c, i).start()
            return carry

        half = n_pl // 2
        lax.fori_loop(half, n_pl, step, 0)
        lax.fori_loop(1, half, step, 0)

    def others(ref, q, c, s_sem, r_sem):
        ref = ref.at[q, c, 1:n_pl]
        return remote(ref, ref, s_sem.at[q, c], r_sem.at[q, c], at(near))

    def scatter(s):
        q = slots[s]
        for c in chunks:
            if s == 1:
                rows_landed(1, c)
            if s >= 2:
                @pl.when(is_end)
                def _():
                    rows_landed(s, c)

            outbox[q, c] = dot(pack[q], rows[q, c]).astype(bf16).reshape(n_pl, pitch, cols_c)
            start_all(dispatch, s, c)
            arrived[q, c, 0] = outbox[q, c, 0]

    def experts(s):
        q = slots[s]
        gate_value = up_value = None
        for c in chunks:
            others(arrived, q, c, d_send, d_recv).wait_recv()
            x = arrived[q, c].reshape(n_slot, cols_c)
            g, u = dot(x, wg[span(c), :]), dot(x, wu[span(c), :])
            gate_value = g if gate_value is None else gate_value + g
            up_value = u if up_value is None else up_value + u
        hidden = (gate_value / (1.0 + jnp.exp(-gate_value)) * up_value).astype(bf16)
        for c in chunks:
            out = dot(hidden, wd[:, span(c)]).astype(bf16)
            arrived[q, c] = out.reshape(n_pl, pitch, cols_c)
            start_all(answer, s, c)
            returned[q, c, 0] = arrived[q, c, 0]

    def home(s, c):
        return remote(part.at[s, c], incoming.at[min(s, 2) - 1, c], p_send.at[s, c],
                      i_recv.at[min(s, 2) - 1, c], at((None, near, mirror, across)[s]))

    def inward(s, c):
        return remote(part.at[s, c], relayed.at[s - 2, c], p_send.at[s, c],
                      m_recv.at[s - 2, c], at(near))

    dims = (((0,), (0,)), ((), ()))

    def gather(s):
        q = slots[s]
        for c in chunks:
            others(returned, q, c, r_send, r_recv).wait_recv()
            back = returned[q, c].reshape(n_slot, cols_c)
            got = lax.dot_general(comb_hi[q], back, dims, preferred_element_type=f32)
            got = got + lax.dot_general(comb_lo[q], back, dims, preferred_element_type=f32)
            if s == 0:
                total[c] = got
            elif s == 1:
                part[s, c] = got.astype(bf16)
                home(s, c).start()
            else:
                @pl.when(is_end)
                def _():
                    part[s, c] = got.astype(bf16)
                    inward(s, c).start()

                @pl.when(is_mid)
                def _():
                    inward(s, c).wait_recv()
                    part[s, c] = (got + relayed[s - 2, c].astype(f32)).astype(bf16)
                    home(s, c).start()

    for c in chunks:
        to_near(c).start()
    for c in chunks:
        to_beyond(c).start()
    scatter(0)
    for copy in tables_far:
        copy.wait()
    for n in range(1, planes):
        route(n, ids_far[n], gate_far[n])
    for w in weights[1:]:
        w.wait()
    experts(0)
    relay(2)
    scatter(1)
    experts(1)
    gather(0)
    scatter(2)
    relay(3)
    gather(1)
    experts(2)
    scatter(3)
    gather(2)
    experts(3)
    gather(3)

    squares = 0.0
    for c in chunks:
        for n in range(2):
            remote(incoming.at[n, c], incoming.at[n, c], p_send.at[1, c], i_recv.at[n, c], at(near)).wait_recv()
        tot = total[c] + incoming[0, c].astype(f32) + incoming[1, c].astype(f32)
        total[c] = tot
        squares = squares + jnp.sum(tot * tot, axis=-1, keepdims=True)
    scale = lax.rsqrt(squares * (1.0 / d_model) + eps_norm)
    for c in chunks:
        out_ref[:, span(c)] = (
            first[:, span(c)].astype(f32) + total[c] * scale * post_ref[:, span(c)]
        ).astype(bf16)

    for kv in (1, 0):
        for t in range(1, planes):
            for up in (1, 0):
                @pl.when(along_ok(up, t))
                def _():
                    along(kv, up, t).wait_send()

        for plane in range(planes):
            for j in range(1, wide):
                aside(kv, plane, j).wait_send()
    for c in chunks:
        to_near(c).wait_send()
        to_beyond(c).wait_send()

        @pl.when(is_mid)
        def _():
            for s in (2, 3):
                pass_on(s, c).wait_send()

        for s in range(planes):
            others(outbox, s, c, d_send, d_recv).wait_send()
            others(arrived, s, c, r_send, r_recv).wait_send()
            if s:
                home(s, c).wait_send()


def shards(
    queries, keys, values, q_gain, k_gain, residual, out_weight, mix_gain, ffn_gain, post_gain,
    expert_ids, expert_gate, w_gate, w_up, w_down,
):
    n_sp = lax.axis_size("sp")
    n_dp = lax.axis_size("dp")
    n_dev = n_sp * n_dp
    tok = queries.shape[1]
    d_model = residual.shape[2]
    d_exp = w_gate.shape[2]
    head = q_gain.shape[0]
    kv_width = keys.shape[2]
    q_width = queries.shape[2]
    top = expert_ids.shape[2]
    cap = 2 * tok * top // n_dev
    pitch = -(-cap // 16) * 16
    wide = n_dp // 2
    planes = n_sp // wide
    n_pl = wide * n_dp
    n_slot = n_pl * pitch
    n_col = 2
    cols_c = d_model // n_col
    vmem = pl.BlockSpec(memory_space=pltpu.VMEM)
    hbm = pl.BlockSpec(memory_space=pl.ANY)
    dma = pltpu.SemaphoreType.DMA
    result = pl.pallas_call(
        functools.partial(kernel, n_sp, n_dp, pitch, n_col),
        out_shape=jax.ShapeDtypeStruct((tok, d_model), bf16),
        in_specs=[vmem] * 15 + [hbm] * 4,
        out_specs=vmem,
        scratch_shapes=[
            pltpu.VMEM((n_sp, tok, kv_width), bf16),
            pltpu.VMEM((n_sp, tok, kv_width), bf16),
            pltpu.VMEM((tok, q_width), bf16),
            pltpu.VMEM((tok, d_model), bf16),
            pltpu.VMEM((planes, n_col, tok, cols_c), bf16),
            pltpu.VMEM((planes, n_col, n_pl, pitch, cols_c), bf16),
            pltpu.VMEM((planes, n_col, n_pl, pitch, cols_c), bf16),
            pltpu.VMEM((planes, n_col, n_pl, pitch, cols_c), bf16),
            pltpu.VMEM((planes, n_slot, tok), bf16),
            pltpu.VMEM((planes, n_slot, tok), bf16),
            pltpu.VMEM((planes, n_slot, tok), bf16),
            pltpu.VMEM((planes, top, tok), jnp.int32),
            pltpu.VMEM((planes, top, tok), f32),
            pltpu.VMEM((planes, n_col, tok, cols_c), bf16),
            pltpu.VMEM((2, n_col, tok, cols_c), bf16),
            pltpu.VMEM((2, n_col, tok, cols_c), bf16),
            pltpu.VMEM((n_col, tok, cols_c), f32),
            pltpu.VMEM((q_width, d_model), bf16),
            pltpu.VMEM((d_model, d_exp), bf16),
            pltpu.VMEM((d_model, d_exp), bf16),
            pltpu.VMEM((d_exp, d_model), bf16),
            dma((4,)),
            dma((2, 2, planes)), dma((2, planes, wide)), dma((2, n_sp)),
            dma((2, planes)), dma((2, planes)),
            dma((planes, n_col)), dma((planes, n_col)),
            dma((planes, n_col)), dma((planes, n_col)), dma((planes, n_col)), dma((planes, n_col)),
            dma((planes, n_col)), dma((2, n_col)), dma((2, n_col)),
        ],
        compiler_params=pltpu.CompilerParams(
            collective_id=0, has_side_effects=True, vmem_limit_bytes=63000000
        ),
    )(
        queries[0], keys[0], values[0], q_gain[None], k_gain[None],
        *tables(n_sp * tok // GRID, head),
        residual[0], mix_gain[None], ffn_gain[None], post_gain[None],
        expert_ids[0].T, expert_gate[0].T,
        out_weight, w_gate[0], w_up[0], w_down[0],
    )
    return result[None]


def solution(mesh):
    tokens = P("dp", "sp", None)
    experts = P(("sp", "dp"), None, None)
    return jax.shard_map(
        shards,
        mesh=mesh,
        in_specs=(tokens, tokens, tokens, P(), P(), tokens, P(), P(), P(), P(), tokens, tokens,
                  experts, experts, experts),
        out_specs=tokens,
        check_vma=False,
    )
```

```python
import functools

import jax
import jax.numpy as jnp
import numpy as np
from jax import lax
from jax.experimental import pallas as pl
from jax.experimental.pallas import tpu as pltpu
from jax.sharding import PartitionSpec as P

GRID = 64
LANES = 128
eps_norm = 1e-06
theta_base = 10000.0
MESH = pl.DeviceIdType.MESH
f32 = jnp.float32
bf16 = jnp.bfloat16


def tables(rows, head_size):
    half = head_size // 2
    lane = np.arange(LANES) % head_size
    pair = lane // 2
    quarter = head_size // 4
    by_row = pair < quarter
    frequency = theta_base ** (-(4.0 * (pair % quarter)) / head_size)
    sign = np.where(lane % 2 == 0, -1.0, 1.0)
    a_row = np.arange(rows)[:, None] * frequency
    a_col = np.arange(GRID)[:, None] * frequency
    out = (
        np.where(by_row, np.cos(a_row), 0.0),
        np.where(by_row, np.sin(a_row) * sign, 0.0),
        np.where(by_row, 0.0, np.cos(a_col)),
        np.where(by_row, 0.0, np.sin(a_col) * sign),
    )
    return [jnp.asarray(t, f32) for t in out]


def rms(x):
    return x * lax.rsqrt(jnp.mean(x * x, axis=-1, keepdims=True) + eps_norm)


def dot(a, b):
    return jnp.dot(a, b, preferred_element_type=f32)


def kernel(
    n_sp, n_dp, pitch, n_col,
    *refs,
):
    n_in = 19
    in_hbm, out_ref, in_vmem, refs = refs[:n_in], refs[n_in], refs[n_in + 1 : 2 * n_in + 1], refs[2 * n_in + 1 :]
    (
        k_ref, kg_ref, cr_ref, sr_ref, cc_ref, sc_ref, v_ref, q_ref, qg_ref, ids_ref, gate_ref,
        res_ref, mix_ref, ffn_ref, post_ref, wo, wg, wu, wd,
    ) = in_vmem
    (
        kbuf, vbuf, att, first, rows, outbox, arrived, returned, pack, comb_hi, comb_lo,
        ids_far, gate_far, part, relayed, incoming, total, inner, hidden, held,
        w_sem,
        kz_send, ky_send, k_recv, t_send, t_recv, z_send, z_recv,
        d_send, d_recv, r_send, r_recv, p_send, m_recv, i_recv,
    ) = refs
    sp = lax.axis_index("sp")
    dp = lax.axis_index("dp")
    tok, q_width = q_ref.shape
    kv_width = k_ref.shape[1]
    head = qg_ref.shape[1]
    d_model = res_ref.shape[1]
    heads_q, heads_kv = q_width // head, kv_width // head
    group = heads_q // heads_kv

    wide = n_dp // 2
    planes = n_sp // wide
    n_pl = wide * n_dp
    n_slot = n_pl * pitch
    cols_c = d_model // n_col
    z = sp // wide
    y = sp % wide
    mid = (z // 2 + z % 2) % 2
    near = z + 1 - 2 * (z % 2)
    across = (z + 2) % planes
    mirror = planes - 1 - z
    is_mid = mid == 1
    is_end = mid == 0

    def at(plane):
        return plane * wide + y, dp

    def peer(i):
        return z * wide + lax.rem(y + i // n_dp, wide), lax.rem(dp + i % n_dp, n_dp)

    def source(i):
        return z * wide + lax.rem(y + wide - i // n_dp, wide), lax.rem(dp + n_dp - i % n_dp, n_dp)

    def remote(src, dst, s_sem, r_sem, to):
        return pltpu.make_async_remote_copy(src, dst, s_sem, r_sem, device_id=to, device_id_type=MESH)

    barrier = pltpu.get_barrier_semaphore()
    up_ok, down_ok = z < planes - 1, z > 0

    @pl.when(up_ok)
    def _():
        pl.semaphore_signal(barrier, inc=1, device_id=at(z + 1), device_id_type=MESH)

    @pl.when(down_ok)
    def _():
        pl.semaphore_signal(barrier, inc=1, device_id=at(z - 1), device_id_type=MESH)

    def greet(i, c):
        pl.semaphore_signal(barrier, inc=1, device_id=peer(i), device_id_type=MESH)
        return c

    lax.fori_loop(1, n_pl, greet, 0)

    loads = [
        pltpu.make_async_copy(src, dst, w_sem.at[n]) for n, (src, dst) in enumerate(zip(in_hbm, in_vmem))
    ]
    for load in loads:
        load.start()
    weights = loads[15:]

    lane = lax.broadcasted_iota(jnp.int32, (tok, LANES), 1)
    even = lane % 2 == 0
    low = lane % (2 * head) < head
    same = (
        lax.broadcasted_iota(jnp.int32, (LANES, LANES), 0) // head
        == lax.broadcasted_iota(jnp.int32, (LANES, LANES), 1) // head
    ).astype(bf16)
    for load in loads[:7]:
        load.wait()
    per_dev = tok // GRID
    cos_t = jnp.concatenate(
        [cc_ref[...] + cr_ref[pl.ds(sp * per_dev + u, 1), :] for u in range(per_dev)], axis=0
    )
    sin_t = jnp.concatenate(
        [sc_ref[...] + sr_ref[pl.ds(sp * per_dev + u, 1), :] for u in range(per_dev)], axis=0
    )

    def turn(x, gain):
        x = x.astype(f32)
        square = x * x
        hi = square.astype(bf16)
        lo = (square - hi.astype(f32)).astype(bf16)
        mean = (dot(hi, same) + dot(lo, same)) * (1.0 / head)
        x = x * lax.rsqrt(mean + eps_norm) * gain
        swapped = jnp.where(even, pltpu.roll(x, LANES - 1, 1), pltpu.roll(x, 1, 1))
        return x * cos_t + swapped * sin_t

    k_gain = jnp.concatenate([kg_ref[...]] * (LANES // head), axis=1)
    for load in loads[7:11]:
        load.wait()
    q_gain = jnp.concatenate([qg_ref[...]] * (LANES // head), axis=1)
    for c in range(kv_width // LANES):
        cols = slice(c * LANES, (c + 1) * LANES)
        kbuf[sp, :, cols] = turn(k_ref[:, cols], k_gain).astype(bf16)
    vbuf[sp] = v_ref[...]

    pl.semaphore_wait(barrier, n_pl - 1 + jnp.minimum(z, 1) + jnp.minimum(planes - 1 - z, 1))

    bufs = (kbuf, vbuf)

    def block(kv, plane, own):
        return v_ref if own and kv == 1 else bufs[kv].at[plane * wide + y]

    def along(kv, up, t):
        plane, to = (z - (t - 1), z + 1) if up else (z + (t - 1), z - 1)
        return remote(
            block(kv, plane, t == 1), bufs[kv].at[plane * wide + y],
            kz_send.at[kv, up, t], k_recv.at[kv, plane * wide + y], at(to),
        )

    def aside(kv, plane, j, own=False):
        return remote(
            block(kv, plane, own), bufs[kv].at[plane * wide + y],
            ky_send.at[kv, plane, j], k_recv.at[kv, plane * wide + y],
            (z * wide + lax.rem(y + j, wide), dp),
        )

    def landed(kv, where):
        ref = bufs[kv].at[where]
        remote(ref, ref, kz_send.at[kv, 0, 0], k_recv.at[kv, where], at(z)).wait_recv()

    def along_ok(up, t):
        return (z >= t - 1) & up_ok if up else (z + t - 1 < planes) & down_ok

    def along_start(kv, up, t):
        @pl.when(along_ok(up, t))
        def _():
            along(kv, up, t).start()

    for kv in (1, 0):
        along_start(kv, 1, 1)
        along_start(kv, 0, 1)
        for j in range(1, wide):
            aside(kv, z, j, own=True).start()

    q_rows = [[] for _ in range(heads_kv)]
    per_chunk = LANES // head

    def turn_q(c):
        x = turn(q_ref[:, c * LANES : (c + 1) * LANES], q_gain) * head ** (-0.5)
        for part_ in range(per_chunk):
            kv = (c * per_chunk + part_) // group
            want = kv % per_chunk
            yq = x if part_ == want else pltpu.roll(x, head, 1)
            keep = low if want == 0 else jnp.logical_not(low)
            q_rows[kv].append(jnp.where(keep, yq, 0.0).astype(bf16))

    order = lax.broadcasted_iota(jnp.int32, (n_pl, tok), 0)
    e_iota = z * n_pl + (y + order // n_dp) % wide * n_dp + (dp + order % n_dp) % n_dp
    before = (
        lax.broadcasted_iota(jnp.int32, (tok, tok), 0) < lax.broadcasted_iota(jnp.int32, (tok, tok), 1)
    ).astype(bf16)
    spread = (
        lax.broadcasted_iota(jnp.int32, (n_slot, n_pl), 0) // pitch
        == lax.broadcasted_iota(jnp.int32, (n_slot, n_pl), 1)
    ).astype(bf16)
    place = (lax.broadcasted_iota(jnp.int32, (n_slot, tok), 0) % pitch + 1).astype(f32)

    def route(n, ids, gates):
        hit0 = (e_iota == ids[0:1, :]).astype(f32)
        hit1 = (e_iota == ids[1:2, :]).astype(f32)
        hits = hit0 + hit1
        rank = dot(hits.astype(bf16), before)
        mark = (hits * (rank + 1.0)).astype(bf16)
        chosen = dot(spread, mark) == place
        pack[n] = chosen.astype(f32).astype(bf16)
        g_hi = gates.astype(bf16).astype(f32)
        g_lo = gates - g_hi
        for dst, piece_ in ((comb_hi, g_hi), (comb_lo, g_lo)):
            both = (hit0 * piece_[0:1, :] + hit1 * piece_[1:2, :]).astype(bf16)
            dst[n] = jnp.where(chosen, dot(spread, both), 0.0).astype(bf16)

    n_turn = q_width // LANES
    done = 0
    for t in range(1, planes):
        upto = n_turn * t // (planes - 1)
        for c in range(done, upto):
            turn_q(c)
        done = upto
        if t == planes - 1:
            route(0, ids_ref[...], gate_ref[...])
        for kv in (1, 0):
            for up in (1, 0):
                plane = z - t if up else z + t

                @pl.when((z >= t) if up else (z + t < planes))
                def _():
                    landed(kv, plane * wide + y)
                    if t < planes - 1:
                        along_start(kv, up, t + 1)
                    for j in range(1, wide):
                        aside(kv, plane, j).start()

    def tables_to(n, to):
        return [
            remote(ids_ref, ids_far.at[n], t_send.at[0, n], t_recv.at[0, n], at(to)),
            remote(gate_ref, gate_far.at[n], t_send.at[1, n], t_recv.at[1, n], at(to)),
        ]

    tables_far = [c for n, to in ((1, near), (2, across), (3, mirror)) for c in tables_to(n, to)]
    for copy in tables_far:
        copy.start()

    for kv in (1, 0):
        for plane in range(planes):
            for j in range(1, wide):
                landed(kv, plane * wide + lax.rem(y + wide - j, wide))

    keys = n_sp * tok
    outs = {}
    for kv in range(heads_kv):
        cols = slice(kv // per_chunk * LANES, (kv // per_chunk + 1) * LANES)
        k_all = kbuf[:, :, cols].reshape(keys, LANES)
        v_all = vbuf[:, :, cols].reshape(keys, LANES)
        for part_ in range(group):
            s = lax.dot_general(
                q_rows[kv][part_], k_all, (((1,), (1,)), ((), ())), preferred_element_type=f32
            )
            p = jnp.exp(s - jnp.max(s, axis=-1, keepdims=True))
            denom = jnp.sum(p, axis=-1, keepdims=True)
            outs[kv * group + part_] = dot(p.astype(bf16), v_all) / denom
    for c in range(q_width // LANES):
        piece = None
        for part_ in range(per_chunk):
            h = c * per_chunk + part_
            have = (h // group) % per_chunk
            yo = outs[h] if part_ == have else pltpu.roll(outs[h], head, 1)
            piece = yo if piece is None else jnp.where(low, piece, yo)
        att[:, c * LANES : (c + 1) * LANES] = piece.astype(bf16)

    weights[0].wait()
    for load in loads[11:15]:
        load.wait()
    projected = dot(att[...], wo[...])
    mixed = (res_ref[...].astype(f32) + rms(projected) * mix_ref[...]).astype(bf16)
    first[...] = mixed
    normed = (rms(mixed.astype(f32)) * ffn_ref[...]).astype(bf16)
    chunks = range(n_col)

    def span(c):
        return slice(c * cols_c, (c + 1) * cols_c)

    for c in chunks:
        rows[0, c] = normed[:, span(c)]

    slots = (0, 1, 2 + mid, 3 - mid)

    def to_near(c):
        return remote(rows.at[0, c], rows.at[1, c], z_send.at[0, c], z_recv.at[1, c], at(near))

    def to_mirror(n, c):
        return remote(
            rows.at[n, c], rows.at[3 - n, c], z_send.at[1 + 3 * n, c], z_recv.at[3 - n, c], at(mirror)
        )

    def pass_on(s, c):
        return remote(
            rows.at[5 - s, c], rows.at[s, c], z_send.at[s, c], z_recv.at[s, c], at(near)
        )

    def rows_landed(slot, c):
        remote(
            rows.at[slot, c], rows.at[slot, c], z_send.at[0, c], z_recv.at[slot, c], at(near)
        ).wait_recv()

    def relay(s, c):
        @pl.when(is_mid)
        def _():
            rows_landed(slots[s], c)
            pass_on(s, c).start()

    def dispatch(s, c, i):
        q = slots[s]
        return remote(
            outbox.at[q, c, i], arrived.at[q, c, i], d_send.at[q, c], d_recv.at[q, c], peer(i)
        )

    def answer(s, c, i):
        q = slots[s]
        return remote(
            arrived.at[q, c, i], returned.at[q, c, i], r_send.at[q, c], r_recv.at[q, c], source(i)
        )

    def start_all(make, s, c):
        def step(i, carry):
            make(s, c, i).start()
            return carry

        half = n_pl // 2
        lax.fori_loop(half, n_pl, step, 0)
        lax.fori_loop(1, half, step, 0)

    def others(ref, q, c, s_sem, r_sem):
        ref = ref.at[q, c, 1:n_pl]
        return remote(ref, ref, s_sem.at[q, c], r_sem.at[q, c], at(near))

    def scatter(s, c):
        q = slots[s]
        if s == 1:
            rows_landed(1, c)

            @pl.when(is_mid)
            def _():
                to_mirror(1, c).start()

        if s >= 2:
            @pl.when(is_end)
            def _():
                rows_landed(s, c)

        outbox[q, c] = dot(pack[q], rows[q, c]).astype(bf16).reshape(n_pl, pitch, cols_c)
        start_all(dispatch, s, c)
        arrived[q, c, 0] = outbox[q, c, 0]

    def widen(s, c):
        q = slots[s]
        others(arrived, q, c, d_send, d_recv).wait_recv()
        x = arrived[q, c].reshape(n_slot, cols_c)
        for n, w in enumerate((wg, wu)):
            got = dot(x, w[span(c), :])
            inner[s % 2, n] = got if c == 0 else inner[s % 2, n] + got

    def hide(s):
        gate_value, up_value = inner[s % 2, 0], inner[s % 2, 1]
        hidden[s % 2] = (gate_value / (1.0 + jnp.exp(-gate_value)) * up_value).astype(bf16)

    def narrow(s, c):
        q = slots[s]
        out = dot(hidden[s % 2], wd[:, span(c)]).astype(bf16)
        arrived[q, c] = out.reshape(n_pl, pitch, cols_c)
        start_all(answer, s, c)
        returned[q, c, 0] = arrived[q, c, 0]

    def home(s, c):
        return remote(part.at[s, c], incoming.at[min(s, 2) - 1, c], p_send.at[s, c],
                      i_recv.at[min(s, 2) - 1, c], at((None, near, mirror, across)[s]))

    def inward(s, c):
        return remote(part.at[s, c], relayed.at[s - 2, c], p_send.at[s, c],
                      m_recv.at[s - 2, c], at(near))

    dims = (((0,), (0,)), ((), ()))

    def gather(s, c):
        q = slots[s]
        others(returned, q, c, r_send, r_recv).wait_recv()
        back = returned[q, c].reshape(n_slot, cols_c)
        got = lax.dot_general(comb_hi[q], back, dims, preferred_element_type=f32)
        got = got + lax.dot_general(comb_lo[q], back, dims, preferred_element_type=f32)
        if s == 0:
            total[c] = got
        elif s == 1:
            part[s, c] = got.astype(bf16)
            home(s, c).start()
        else:
            @pl.when(is_end)
            def _():
                part[s, c] = got.astype(bf16)
                inward(s, c).start()

            @pl.when(is_mid)
            def _():
                held[s - 2, c] = got

    def merge(s, c):
        @pl.when(is_mid)
        def _():
            inward(s, c).wait_recv()
            part[s, c] = (held[s - 2, c] + relayed[s - 2, c].astype(f32)).astype(bf16)
            home(s, c).start()

    for c in chunks:
        to_near(c).start()

    @pl.when(is_mid)
    def _():
        for c in chunks:
            to_mirror(0, c).start()

    for c in chunks:
        scatter(0, c)
    for copy in tables_far:
        copy.wait()
    for n in range(1, planes):
        route(n, ids_far[n], gate_far[n])
    for w in weights[1:]:
        w.wait()
    relay(2, 1)
    widen(0, 0)
    scatter(1, 0)
    scatter(1, 1)
    widen(0, 1)
    widen(0, 2)
    widen(0, 3)
    hide(0)
    narrow(0, 2)
    relay(2, 0)
    widen(1, 0)
    scatter(1, 2)
    narrow(0, 3)
    widen(1, 1)
    relay(2, 2)
    scatter(1, 3)
    relay(2, 3)
    narrow(0, 0)
    widen(1, 2)
    relay(3, 0)
    scatter(2, 1)
    relay(3, 1)
    widen(1, 3)
    narrow(0, 1)
    hide(1)
    narrow(1, 3)
    scatter(2, 0)
    gather(0, 3)
    narrow(1, 2)
    scatter(2, 2)
    relay(3, 2)
    relay(3, 3)
    narrow(1, 0)
    gather(1, 3)
    scatter(2, 3)
    gather(1, 2)
    widen(2, 0)
    narrow(1, 1)
    gather(1, 0)
    scatter(3, 0)
    gather(0, 2)
    widen(2, 1)
    widen(2, 2)
    widen(2, 3)
    hide(2)
    narrow(2, 2)
    gather(1, 1)
    scatter(3, 1)
    widen(3, 0)
    narrow(2, 3)
    scatter(3, 2)
    narrow(2, 0)
    gather(2, 2)
    widen(3, 1)
    scatter(3, 3)
    gather(2, 3)
    merge(2, 2)
    narrow(2, 1)
    merge(2, 3)
    gather(0, 0)
    gather(2, 0)
    gather(0, 1)
    merge(2, 0)
    widen(3, 2)
    widen(3, 3)
    hide(3)
    narrow(3, 0)
    gather(2, 1)
    narrow(3, 1)
    merge(2, 1)
    narrow(3, 2)
    gather(3, 0)
    merge(3, 0)
    gather(3, 1)
    narrow(3, 3)
    merge(3, 1)
    gather(3, 2)
    gather(3, 3)
    merge(3, 2)
    merge(3, 3)

    squares = 0.0
    for c in chunks:
        for n in range(2):
            remote(incoming.at[n, c], incoming.at[n, c], p_send.at[1, c], i_recv.at[n, c], at(near)).wait_recv()
        tot = total[c] + incoming[0, c].astype(f32) + incoming[1, c].astype(f32)
        total[c] = tot
        squares = squares + jnp.sum(tot * tot, axis=-1, keepdims=True)
    scale = lax.rsqrt(squares * (1.0 / d_model) + eps_norm)
    for c in chunks:
        out_ref[:, span(c)] = (
            first[:, span(c)].astype(f32) + total[c] * scale * post_ref[:, span(c)]
        ).astype(bf16)

    for kv in (1, 0):
        for t in range(1, planes):
            for up in (1, 0):
                @pl.when(along_ok(up, t))
                def _():
                    along(kv, up, t).wait_send()

        for plane in range(planes):
            for j in range(1, wide):
                aside(kv, plane, j).wait_send()
    for c in chunks:
        to_near(c).wait_send()

        @pl.when(is_mid)
        def _():
            for n in (0, 1):
                to_mirror(n, c).wait_send()
            for s in (2, 3):
                pass_on(s, c).wait_send()

        for s in range(planes):
            others(outbox, s, c, d_send, d_recv).wait_send()
            others(arrived, s, c, r_send, r_recv).wait_send()
            if s:
                home(s, c).wait_send()


def shards(
    queries, keys, values, q_gain, k_gain, residual, out_weight, mix_gain, ffn_gain, post_gain,
    expert_ids, expert_gate, w_gate, w_up, w_down,
):
    n_sp = lax.axis_size("sp")
    n_dp = lax.axis_size("dp")
    n_dev = n_sp * n_dp
    tok = queries.shape[1]
    d_model = residual.shape[2]
    d_exp = w_gate.shape[2]
    head = q_gain.shape[0]
    kv_width = keys.shape[2]
    q_width = queries.shape[2]
    top = expert_ids.shape[2]
    cap = 2 * tok * top // n_dev
    pitch = -(-cap // 16) * 16
    wide = n_dp // 2
    planes = n_sp // wide
    n_pl = wide * n_dp
    n_slot = n_pl * pitch
    n_col = 4
    cols_c = d_model // n_col
    vmem = pl.BlockSpec(memory_space=pltpu.VMEM)
    hbm = pl.BlockSpec(memory_space=pl.ANY)
    dma = pltpu.SemaphoreType.DMA
    rows_t, rows_s, cols_t, cols_s = tables(n_sp * tok // GRID, head)
    operands = (
        keys[0], k_gain[None], rows_t, rows_s, cols_t, cols_s, values[0], queries[0], q_gain[None],
        expert_ids[0].T, expert_gate[0].T, residual[0], mix_gain[None], ffn_gain[None], post_gain[None],
        out_weight, w_gate[0], w_up[0], w_down[0],
    )
    result = pl.pallas_call(
        functools.partial(kernel, n_sp, n_dp, pitch, n_col),
        out_shape=jax.ShapeDtypeStruct((tok, d_model), bf16),
        in_specs=[hbm] * len(operands),
        out_specs=vmem,
        scratch_shapes=[pltpu.VMEM(x.shape, x.dtype) for x in operands] + [
            pltpu.VMEM((n_sp, tok, kv_width), bf16),
            pltpu.VMEM((n_sp, tok, kv_width), bf16),
            pltpu.VMEM((tok, q_width), bf16),
            pltpu.VMEM((tok, d_model), bf16),
            pltpu.VMEM((planes, n_col, tok, cols_c), bf16),
            pltpu.VMEM((planes, n_col, n_pl, pitch, cols_c), bf16),
            pltpu.VMEM((planes, n_col, n_pl, pitch, cols_c), bf16),
            pltpu.VMEM((planes, n_col, n_pl, pitch, cols_c), bf16),
            pltpu.VMEM((planes, n_slot, tok), bf16),
            pltpu.VMEM((planes, n_slot, tok), bf16),
            pltpu.VMEM((planes, n_slot, tok), bf16),
            pltpu.VMEM((planes, top, tok), jnp.int32),
            pltpu.VMEM((planes, top, tok), f32),
            pltpu.VMEM((planes, n_col, tok, cols_c), bf16),
            pltpu.VMEM((2, n_col, tok, cols_c), bf16),
            pltpu.VMEM((2, n_col, tok, cols_c), bf16),
            pltpu.VMEM((n_col, tok, cols_c), f32),
            pltpu.VMEM((2, 2, n_slot, d_exp), f32),
            pltpu.VMEM((2, n_slot, d_exp), bf16),
            pltpu.VMEM((2, n_col, tok, cols_c), f32),
            dma((len(operands),)),
            dma((2, 2, planes)), dma((2, planes, wide)), dma((2, n_sp)),
            dma((2, planes)), dma((2, planes)),
            dma((planes + 1, n_col)), dma((planes, n_col)),
            dma((planes, n_col)), dma((planes, n_col)), dma((planes, n_col)), dma((planes, n_col)),
            dma((planes, n_col)), dma((2, n_col)), dma((2, n_col)),
        ],
        compiler_params=pltpu.CompilerParams(
            collective_id=0, has_side_effects=True, vmem_limit_bytes=63000000
        ),
    )(*operands)
    return result[None]


def solution(mesh):
    tokens = P("dp", "sp", None)
    experts = P(("sp", "dp"), None, None)
    return jax.shard_map(
        shards,
        mesh=mesh,
        in_specs=(tokens, tokens, tokens, P(), P(), tokens, P(), P(), P(), P(), tokens, tokens,
                  experts, experts, experts),
        out_specs=tokens,
        check_vma=False,
    )
```

```python
import functools

import jax
import jax.numpy as jnp
import numpy as np
from jax import lax
from jax.experimental import pallas as pl
from jax.experimental.pallas import tpu as pltpu
from jax.sharding import PartitionSpec as P

GRID = 64
LANES = 128
eps_norm = 1e-06
theta_base = 10000.0
MESH = pl.DeviceIdType.MESH
f32 = jnp.float32
bf16 = jnp.bfloat16


def tables(rows, head_size):
    half = head_size // 2
    lane = np.arange(LANES) % head_size
    pair = lane // 2
    quarter = head_size // 4
    by_row = pair < quarter
    frequency = theta_base ** (-(4.0 * (pair % quarter)) / head_size)
    sign = np.where(lane % 2 == 0, -1.0, 1.0)
    a_row = np.arange(rows)[:, None] * frequency
    a_col = np.arange(GRID)[:, None] * frequency
    out = (
        np.where(by_row, np.cos(a_row), 0.0),
        np.where(by_row, np.sin(a_row) * sign, 0.0),
        np.where(by_row, 0.0, np.cos(a_col)),
        np.where(by_row, 0.0, np.sin(a_col) * sign),
    )
    return [jnp.asarray(t, f32) for t in out]


def rms(x):
    return x * lax.rsqrt(jnp.mean(x * x, axis=-1, keepdims=True) + eps_norm)


def dot(a, b):
    return jnp.dot(a, b, preferred_element_type=f32)


def kernel(
    n_sp, n_dp, pitch, n_col,
    *refs,
):
    n_in = 19
    in_hbm, out_ref, in_vmem, refs = refs[:n_in], refs[n_in], refs[n_in + 1 : 2 * n_in + 1], refs[2 * n_in + 1 :]
    (
        k_ref, kg_ref, cr_ref, sr_ref, cc_ref, sc_ref, v_ref, q_ref, qg_ref, ids_ref, gate_ref,
        res_ref, mix_ref, ffn_ref, post_ref, wo, wg, wu, wd,
    ) = in_vmem
    (
        kbuf, vbuf, att, first, rows, outbox, arrived, returned, pack, comb_hi, comb_lo,
        ids_far, gate_far, part, relayed, incoming, total, inner, hidden, held,
        w_sem,
        kz_send, ky_send, k_recv, t_send, t_recv, z_send, z_recv,
        d_send, d_recv, r_send, r_recv, p_send, m_recv, i_recv,
    ) = refs
    sp = lax.axis_index("sp")
    dp = lax.axis_index("dp")
    tok, q_width = q_ref.shape
    kv_width = k_ref.shape[1]
    head = qg_ref.shape[1]
    d_model = res_ref.shape[1]
    heads_q, heads_kv = q_width // head, kv_width // head
    group = heads_q // heads_kv

    wide = n_dp // 2
    planes = n_sp // wide
    n_pl = wide * n_dp
    n_slot = n_pl * pitch
    cols_c = d_model // n_col
    z = sp // wide
    y = sp % wide
    mid = (z // 2 + z % 2) % 2
    near = z + 1 - 2 * (z % 2)
    across = (z + 2) % planes
    mirror = planes - 1 - z
    is_mid = mid == 1
    is_end = mid == 0

    def at(plane):
        return plane * wide + y, dp

    def peer(i):
        return z * wide + lax.rem(y + i // n_dp, wide), lax.rem(dp + i % n_dp, n_dp)

    def source(i):
        return z * wide + lax.rem(y + wide - i // n_dp, wide), lax.rem(dp + n_dp - i % n_dp, n_dp)

    def remote(src, dst, s_sem, r_sem, to):
        return pltpu.make_async_remote_copy(src, dst, s_sem, r_sem, device_id=to, device_id_type=MESH)

    barrier = pltpu.get_barrier_semaphore()
    up_ok, down_ok = z < planes - 1, z > 0

    @pl.when(up_ok)
    def _():
        pl.semaphore_signal(barrier, inc=1, device_id=at(z + 1), device_id_type=MESH)

    @pl.when(down_ok)
    def _():
        pl.semaphore_signal(barrier, inc=1, device_id=at(z - 1), device_id_type=MESH)

    def greet(i, c):
        pl.semaphore_signal(barrier, inc=1, device_id=peer(i), device_id_type=MESH)
        return c

    lax.fori_loop(1, n_pl, greet, 0)

    loads = [
        pltpu.make_async_copy(src, dst, w_sem.at[n]) for n, (src, dst) in enumerate(zip(in_hbm, in_vmem))
    ]
    for load in loads:
        load.start()
    weights = loads[15:]

    lane = lax.broadcasted_iota(jnp.int32, (tok, LANES), 1)
    even = lane % 2 == 0
    low = lane % (2 * head) < head
    same = (
        lax.broadcasted_iota(jnp.int32, (LANES, LANES), 0) // head
        == lax.broadcasted_iota(jnp.int32, (LANES, LANES), 1) // head
    ).astype(bf16)
    for load in loads[:7]:
        load.wait()
    per_dev = tok // GRID
    cos_t = jnp.concatenate(
        [cc_ref[...] + cr_ref[pl.ds(sp * per_dev + u, 1), :] for u in range(per_dev)], axis=0
    )
    sin_t = jnp.concatenate(
        [sc_ref[...] + sr_ref[pl.ds(sp * per_dev + u, 1), :] for u in range(per_dev)], axis=0
    )

    def turn(x, gain):
        x = x.astype(f32)
        square = x * x
        hi = square.astype(bf16)
        lo = (square - hi.astype(f32)).astype(bf16)
        mean = (dot(hi, same) + dot(lo, same)) * (1.0 / head)
        x = x * lax.rsqrt(mean + eps_norm) * gain
        swapped = jnp.where(even, pltpu.roll(x, LANES - 1, 1), pltpu.roll(x, 1, 1))
        return x * cos_t + swapped * sin_t

    k_gain = jnp.concatenate([kg_ref[...]] * (LANES // head), axis=1)
    for load in loads[7:11]:
        load.wait()
    q_gain = jnp.concatenate([qg_ref[...]] * (LANES // head), axis=1)
    for c in range(kv_width // LANES):
        cols = slice(c * LANES, (c + 1) * LANES)
        kbuf[sp, :, cols] = turn(k_ref[:, cols], k_gain).astype(bf16)
    vbuf[sp] = v_ref[...]

    pl.semaphore_wait(barrier, n_pl - 1 + jnp.minimum(z, 1) + jnp.minimum(planes - 1 - z, 1))

    bufs = (kbuf, vbuf)

    def block(kv, plane, own):
        return v_ref if own and kv == 1 else bufs[kv].at[plane * wide + y]

    def along(kv, up, t):
        plane, to = (z - (t - 1), z + 1) if up else (z + (t - 1), z - 1)
        return remote(
            block(kv, plane, t == 1), bufs[kv].at[plane * wide + y],
            kz_send.at[kv, up, t], k_recv.at[kv, plane * wide + y], at(to),
        )

    def aside(kv, plane, j, own=False):
        return remote(
            block(kv, plane, own), bufs[kv].at[plane * wide + y],
            ky_send.at[kv, plane, j], k_recv.at[kv, plane * wide + y],
            (z * wide + lax.rem(y + j, wide), dp),
        )

    def landed(kv, where):
        ref = bufs[kv].at[where]
        remote(ref, ref, kz_send.at[kv, 0, 0], k_recv.at[kv, where], at(z)).wait_recv()

    def along_ok(up, t):
        return (z >= t - 1) & up_ok if up else (z + t - 1 < planes) & down_ok

    def along_start(kv, up, t):
        @pl.when(along_ok(up, t))
        def _():
            along(kv, up, t).start()

    for kv in (1, 0):
        along_start(kv, 1, 1)
        along_start(kv, 0, 1)
        for j in range(1, wide):
            aside(kv, z, j, own=True).start()

    q_rows = [[] for _ in range(heads_kv)]
    per_chunk = LANES // head

    def turn_q(c):
        x = turn(q_ref[:, c * LANES : (c + 1) * LANES], q_gain) * head ** (-0.5)
        for part_ in range(per_chunk):
            kv = (c * per_chunk + part_) // group
            want = kv % per_chunk
            yq = x if part_ == want else pltpu.roll(x, head, 1)
            keep = low if want == 0 else jnp.logical_not(low)
            q_rows[kv].append(jnp.where(keep, yq, 0.0).astype(bf16))

    order = lax.broadcasted_iota(jnp.int32, (n_pl, tok), 0)
    e_iota = z * n_pl + (y + order // n_dp) % wide * n_dp + (dp + order % n_dp) % n_dp
    before = (
        lax.broadcasted_iota(jnp.int32, (tok, tok), 0) < lax.broadcasted_iota(jnp.int32, (tok, tok), 1)
    ).astype(bf16)
    spread = (
        lax.broadcasted_iota(jnp.int32, (n_slot, n_pl), 0) // pitch
        == lax.broadcasted_iota(jnp.int32, (n_slot, n_pl), 1)
    ).astype(bf16)
    place = (lax.broadcasted_iota(jnp.int32, (n_slot, tok), 0) % pitch + 1).astype(f32)

    def route(n, ids, gates):
        hit0 = (e_iota == ids[0:1, :]).astype(f32)
        hit1 = (e_iota == ids[1:2, :]).astype(f32)
        hits = hit0 + hit1
        rank = dot(hits.astype(bf16), before)
        mark = (hits * (rank + 1.0)).astype(bf16)
        chosen = dot(spread, mark) == place
        pack[n] = chosen.astype(f32).astype(bf16)
        g_hi = gates.astype(bf16).astype(f32)
        g_lo = gates - g_hi
        for dst, piece_ in ((comb_hi, g_hi), (comb_lo, g_lo)):
            both = (hit0 * piece_[0:1, :] + hit1 * piece_[1:2, :]).astype(bf16)
            dst[n] = jnp.where(chosen, dot(spread, both), 0.0).astype(bf16)

    n_turn = q_width // LANES
    done = 0
    for t in range(1, planes):
        upto = n_turn * t // (planes - 1)
        for c in range(done, upto):
            turn_q(c)
        done = upto
        if t == planes - 1:
            route(0, ids_ref[...], gate_ref[...])
        for kv in (1, 0):
            for up in (1, 0):
                plane = z - t if up else z + t

                @pl.when((z >= t) if up else (z + t < planes))
                def _():
                    landed(kv, plane * wide + y)
                    if t < planes - 1:
                        along_start(kv, up, t + 1)
                    for j in range(1, wide):
                        aside(kv, plane, j).start()

    def tables_to(n, to):
        return [
            remote(ids_ref, ids_far.at[n], t_send.at[0, n], t_recv.at[0, n], at(to)),
            remote(gate_ref, gate_far.at[n], t_send.at[1, n], t_recv.at[1, n], at(to)),
        ]

    tables_far = [c for n, to in ((1, near), (2, across), (3, mirror)) for c in tables_to(n, to)]
    for copy in tables_far:
        copy.start()

    for kv in (1, 0):
        for plane in range(planes):
            for j in range(1, wide):
                landed(kv, plane * wide + lax.rem(y + wide - j, wide))

    keys = n_sp * tok
    many = group if group * tok * keys <= 1 << 19 else 1
    outs = {}
    for kv in range(heads_kv):
        cols = slice(kv // per_chunk * LANES, (kv // per_chunk + 1) * LANES)
        k_all = kbuf[:, :, cols].reshape(keys, LANES)
        v_all = vbuf[:, :, cols].reshape(keys, LANES)
        for first_ in range(0, group, many):
            q_all = jnp.concatenate(q_rows[kv][first_ : first_ + many], axis=0)
            s = lax.dot_general(
                q_all, k_all, (((1,), (1,)), ((), ())), preferred_element_type=f32
            )
            p = jnp.exp(s - jnp.max(s, axis=-1, keepdims=True))
            out = dot(p.astype(bf16), v_all) / jnp.sum(p, axis=-1, keepdims=True)
            for n in range(many):
                outs[kv * group + first_ + n] = out[n * tok : (n + 1) * tok]
    for c in range(q_width // LANES):
        piece = None
        for part_ in range(per_chunk):
            h = c * per_chunk + part_
            have = (h // group) % per_chunk
            yo = outs[h] if part_ == have else pltpu.roll(outs[h], head, 1)
            piece = yo if piece is None else jnp.where(low, piece, yo)
        att[:, c * LANES : (c + 1) * LANES] = piece.astype(bf16)

    weights[0].wait()
    for load in loads[11:15]:
        load.wait()
    projected = dot(att[...], wo[...])
    mixed = (res_ref[...].astype(f32) + rms(projected) * mix_ref[...]).astype(bf16)
    first[...] = mixed
    normed = (rms(mixed.astype(f32)) * ffn_ref[...]).astype(bf16)
    chunks = range(n_col)

    def span(c):
        return slice(c * cols_c, (c + 1) * cols_c)

    for c in chunks:
        rows[0, c] = normed[:, span(c)]

    slots = (0, 1, 2 + mid, 3 - mid)

    def to_near(c):
        return remote(rows.at[0, c], rows.at[1, c], z_send.at[0, c], z_recv.at[1, c], at(near))

    def to_mirror(n, c):
        return remote(
            rows.at[n, c], rows.at[3 - n, c], z_send.at[1 + 3 * n, c], z_recv.at[3 - n, c], at(mirror)
        )

    def pass_on(s, c):
        return remote(
            rows.at[5 - s, c], rows.at[s, c], z_send.at[s, c], z_recv.at[s, c], at(near)
        )

    def rows_landed(slot, c):
        remote(
            rows.at[slot, c], rows.at[slot, c], z_send.at[0, c], z_recv.at[slot, c], at(near)
        ).wait_recv()

    def relay(s, c):
        @pl.when(is_mid)
        def _():
            rows_landed(slots[s], c)
            pass_on(s, c).start()

    def dispatch(s, c, i):
        q = slots[s]
        return remote(
            outbox.at[q, c, i], arrived.at[q, c, i], d_send.at[q, c], d_recv.at[q, c], peer(i)
        )

    def answer(s, c, i):
        q = slots[s]
        return remote(
            arrived.at[q, c, i], returned.at[q, c, i], r_send.at[q, c], r_recv.at[q, c], source(i)
        )

    def start_all(make, s, c):
        def step(i, carry):
            make(s, c, i).start()
            return carry

        half = n_pl // 2
        lax.fori_loop(half, n_pl, step, 0)
        lax.fori_loop(1, half, step, 0)

    def others(ref, q, c, s_sem, r_sem):
        ref = ref.at[q, c, 1:n_pl]
        return remote(ref, ref, s_sem.at[q, c], r_sem.at[q, c], at(near))

    def scatter(s, c):
        q = slots[s]
        if s == 1:
            rows_landed(1, c)

            @pl.when(is_mid)
            def _():
                to_mirror(1, c).start()

        if s >= 2:
            @pl.when(is_end)
            def _():
                rows_landed(s, c)

        outbox[q, c] = dot(pack[q], rows[q, c]).astype(bf16).reshape(n_pl, pitch, cols_c)
        start_all(dispatch, s, c)
        arrived[q, c, 0] = outbox[q, c, 0]

    def widen(s, c):
        q = slots[s]
        others(arrived, q, c, d_send, d_recv).wait_recv()
        x = arrived[q, c].reshape(n_slot, cols_c)
        for n, w in enumerate((wg, wu)):
            got = dot(x, w[span(c), :])
            inner[s % 2, n] = got if c == 0 else inner[s % 2, n] + got

    def hide(s):
        gate_value, up_value = inner[s % 2, 0], inner[s % 2, 1]
        hidden[s % 2] = (gate_value / (1.0 + jnp.exp(-gate_value)) * up_value).astype(bf16)

    def narrow(s, c):
        q = slots[s]
        out = dot(hidden[s % 2], wd[:, span(c)]).astype(bf16)
        arrived[q, c] = out.reshape(n_pl, pitch, cols_c)
        start_all(answer, s, c)
        returned[q, c, 0] = arrived[q, c, 0]

    def home(s, c):
        return remote(part.at[s, c], incoming.at[min(s, 2) - 1, c], p_send.at[s, c],
                      i_recv.at[min(s, 2) - 1, c], at((None, near, mirror, across)[s]))

    def inward(s, c):
        return remote(part.at[s, c], relayed.at[s - 2, c], p_send.at[s, c],
                      m_recv.at[s - 2, c], at(near))

    dims = (((0,), (0,)), ((), ()))

    def gather(s, c):
        q = slots[s]
        others(returned, q, c, r_send, r_recv).wait_recv()
        back = returned[q, c].reshape(n_slot, cols_c)
        got = lax.dot_general(comb_hi[q], back, dims, preferred_element_type=f32)
        got = got + lax.dot_general(comb_lo[q], back, dims, preferred_element_type=f32)
        if s == 0:
            total[c] = got
        elif s == 1:
            part[s, c] = got.astype(bf16)
            home(s, c).start()
        else:
            @pl.when(is_end)
            def _():
                part[s, c] = got.astype(bf16)
                inward(s, c).start()

            @pl.when(is_mid)
            def _():
                held[s - 2, c] = got

    def merge(s, c):
        @pl.when(is_mid)
        def _():
            inward(s, c).wait_recv()
            part[s, c] = (held[s - 2, c] + relayed[s - 2, c].astype(f32)).astype(bf16)
            home(s, c).start()

    for c in chunks:
        to_near(c).start()

    @pl.when(is_mid)
    def _():
        for c in chunks:
            to_mirror(0, c).start()

    for c in chunks:
        scatter(0, c)
    for copy in tables_far:
        copy.wait()
    for n in range(1, planes):
        route(n, ids_far[n], gate_far[n])
    for w in weights[1:]:
        w.wait()
    relay(2, 1)
    widen(0, 0)
    scatter(1, 0)
    scatter(1, 1)
    widen(0, 1)
    widen(0, 2)
    widen(0, 3)
    hide(0)
    narrow(0, 2)
    relay(2, 0)
    widen(1, 0)
    scatter(1, 2)
    narrow(0, 3)
    widen(1, 1)
    relay(2, 2)
    scatter(1, 3)
    relay(2, 3)
    narrow(0, 0)
    widen(1, 2)
    relay(3, 0)
    scatter(2, 1)
    relay(3, 1)
    widen(1, 3)
    narrow(0, 1)
    hide(1)
    narrow(1, 3)
    scatter(2, 0)
    gather(0, 3)
    narrow(1, 2)
    scatter(2, 2)
    relay(3, 2)
    relay(3, 3)
    narrow(1, 0)
    gather(1, 3)
    scatter(2, 3)
    gather(1, 2)
    widen(2, 0)
    narrow(1, 1)
    gather(1, 0)
    scatter(3, 0)
    gather(0, 2)
    widen(2, 1)
    widen(2, 2)
    widen(2, 3)
    hide(2)
    narrow(2, 2)
    gather(1, 1)
    scatter(3, 1)
    widen(3, 0)
    narrow(2, 3)
    scatter(3, 2)
    narrow(2, 0)
    gather(2, 2)
    widen(3, 1)
    scatter(3, 3)
    gather(2, 3)
    merge(2, 2)
    narrow(2, 1)
    merge(2, 3)
    gather(0, 0)
    gather(2, 0)
    gather(0, 1)
    merge(2, 0)
    widen(3, 2)
    widen(3, 3)
    hide(3)
    narrow(3, 0)
    gather(2, 1)
    narrow(3, 1)
    merge(2, 1)
    narrow(3, 2)
    gather(3, 0)
    merge(3, 0)
    gather(3, 1)
    narrow(3, 3)
    merge(3, 1)
    gather(3, 2)
    gather(3, 3)
    merge(3, 2)
    merge(3, 3)

    squares = 0.0
    for c in chunks:
        for n in range(2):
            remote(incoming.at[n, c], incoming.at[n, c], p_send.at[1, c], i_recv.at[n, c], at(near)).wait_recv()
        tot = total[c] + incoming[0, c].astype(f32) + incoming[1, c].astype(f32)
        total[c] = tot
        squares = squares + jnp.sum(tot * tot, axis=-1, keepdims=True)
    scale = lax.rsqrt(squares * (1.0 / d_model) + eps_norm)
    for c in chunks:
        out_ref[:, span(c)] = (
            first[:, span(c)].astype(f32) + total[c] * scale * post_ref[:, span(c)]
        ).astype(bf16)

    for kv in (1, 0):
        for t in range(1, planes):
            for up in (1, 0):
                @pl.when(along_ok(up, t))
                def _():
                    along(kv, up, t).wait_send()

        for plane in range(planes):
            for j in range(1, wide):
                aside(kv, plane, j).wait_send()
    for c in chunks:
        to_near(c).wait_send()

        @pl.when(is_mid)
        def _():
            for n in (0, 1):
                to_mirror(n, c).wait_send()
            for s in (2, 3):
                pass_on(s, c).wait_send()

        for s in range(planes):
            others(outbox, s, c, d_send, d_recv).wait_send()
            others(arrived, s, c, r_send, r_recv).wait_send()
            if s:
                home(s, c).wait_send()


def shards(
    queries, keys, values, q_gain, k_gain, residual, out_weight, mix_gain, ffn_gain, post_gain,
    expert_ids, expert_gate, w_gate, w_up, w_down,
):
    n_sp = lax.axis_size("sp")
    n_dp = lax.axis_size("dp")
    n_dev = n_sp * n_dp
    tok = queries.shape[1]
    d_model = residual.shape[2]
    d_exp = w_gate.shape[2]
    head = q_gain.shape[0]
    kv_width = keys.shape[2]
    q_width = queries.shape[2]
    top = expert_ids.shape[2]
    cap = 2 * tok * top // n_dev
    pitch = -(-cap // 16) * 16
    wide = n_dp // 2
    planes = n_sp // wide
    n_pl = wide * n_dp
    n_slot = n_pl * pitch
    n_col = 4
    cols_c = d_model // n_col
    vmem = pl.BlockSpec(memory_space=pltpu.VMEM)
    hbm = pl.BlockSpec(memory_space=pl.ANY)
    dma = pltpu.SemaphoreType.DMA
    rows_t, rows_s, cols_t, cols_s = tables(n_sp * tok // GRID, head)
    operands = (
        keys[0], k_gain[None], rows_t, rows_s, cols_t, cols_s, values[0], queries[0], q_gain[None],
        expert_ids[0].T, expert_gate[0].T, residual[0], mix_gain[None], ffn_gain[None], post_gain[None],
        out_weight, w_gate[0], w_up[0], w_down[0],
    )
    result = pl.pallas_call(
        functools.partial(kernel, n_sp, n_dp, pitch, n_col),
        out_shape=jax.ShapeDtypeStruct((tok, d_model), bf16),
        in_specs=[hbm] * len(operands),
        out_specs=vmem,
        scratch_shapes=[pltpu.VMEM(x.shape, x.dtype) for x in operands] + [
            pltpu.VMEM((n_sp, tok, kv_width), bf16),
            pltpu.VMEM((n_sp, tok, kv_width), bf16),
            pltpu.VMEM((tok, q_width), bf16),
            pltpu.VMEM((tok, d_model), bf16),
            pltpu.VMEM((planes, n_col, tok, cols_c), bf16),
            pltpu.VMEM((planes, n_col, n_pl, pitch, cols_c), bf16),
            pltpu.VMEM((planes, n_col, n_pl, pitch, cols_c), bf16),
            pltpu.VMEM((planes, n_col, n_pl, pitch, cols_c), bf16),
            pltpu.VMEM((planes, n_slot, tok), bf16),
            pltpu.VMEM((planes, n_slot, tok), bf16),
            pltpu.VMEM((planes, n_slot, tok), bf16),
            pltpu.VMEM((planes, top, tok), jnp.int32),
            pltpu.VMEM((planes, top, tok), f32),
            pltpu.VMEM((planes, n_col, tok, cols_c), bf16),
            pltpu.VMEM((2, n_col, tok, cols_c), bf16),
            pltpu.VMEM((2, n_col, tok, cols_c), bf16),
            pltpu.VMEM((n_col, tok, cols_c), f32),
            pltpu.VMEM((2, 2, n_slot, d_exp), f32),
            pltpu.VMEM((2, n_slot, d_exp), bf16),
            pltpu.VMEM((2, n_col, tok, cols_c), f32),
            dma((len(operands),)),
            dma((2, 2, planes)), dma((2, planes, wide)), dma((2, n_sp)),
            dma((2, planes)), dma((2, planes)),
            dma((planes + 1, n_col)), dma((planes, n_col)),
            dma((planes, n_col)), dma((planes, n_col)), dma((planes, n_col)), dma((planes, n_col)),
            dma((planes, n_col)), dma((2, n_col)), dma((2, n_col)),
        ],
        compiler_params=pltpu.CompilerParams(
            collective_id=0, has_side_effects=True, vmem_limit_bytes=63000000
        ),
    )(*operands)
    return result[None]


def solution(mesh):
    tokens = P("dp", "sp", None)
    experts = P(("sp", "dp"), None, None)
    return jax.shard_map(
        shards,
        mesh=mesh,
        in_specs=(tokens, tokens, tokens, P(), P(), tokens, P(), P(), P(), P(), tokens, tokens,
                  experts, experts, experts),
        out_specs=tokens,
        check_vma=False,
    )
```
